32 devices in a mesh: sp: 8 (over z, core), tp: 4 (over y, x).
Axes of the slice: x: 2, y: 2, z: 4, core: 2. Of those that a mesh axis runs over, the one named last changes fastest.
Arguments:
- queries: bfloat16 [2048, 2048], P('sp', 'tp'), may hold values from -6 to 6
- keys: bfloat16 [2048, 256], P('sp'), may hold values from -6 to 6
- values: bfloat16 [2048, 256], P('sp'), may hold values from -6 to 6
- query_gain: float32 [128], replicated, may hold values from 0.1 to 5.5
- key_gain: float32 [128], replicated, may hold values from 0.1 to 5.5
- out_proj: bfloat16 [2048, 2048], P(None, 'tp'), may hold values from -0.125 to 0.125
- expert_norm_scale: float32 [2048], replicated, may hold values from 0.1 to 1.9
- residual: bfloat16 [2048, 2048], P(('sp', 'tp')), may hold values from -6 to 6
- routes: int32 [2048, 2], P(('sp', 'tp')), may hold values from 0 to 7, all different within a row; in each aligned block of 64 rows (0 to 63, 64 to 127, ...) at most 32 rows name the same one
- route_weights: float32 [2048, 2], P(('sp', 'tp')), may hold values from 0.1 to 0.9
- w_gate: bfloat16 [8, 2048, 4096], P('sp', None, 'tp'), may hold values from -0.125 to 0.125
- w_up: bfloat16 [8, 2048, 4096], P('sp', None, 'tp'), may hold values from -0.125 to 0.125
- w_down: bfloat16 [8, 4096, 2048], P('sp', 'tp'), may hold values from -0.09375 to 0.09375
Outputs:
- layer_out: bfloat16 [2048, 2048], P(('sp', 'tp'))
The draws below stay inside these ranges and needn't reach their ends.
Inputs may be any that keep to these rules, and one draw needn't show every extreme that they name: `routes`: in the rows of one device no expert is named by more than 32 rows, a bound that some block reaches; a row names 2 different experts.
All inputs are finite; a program needn't handle non-finite values.
Results may differ from the reference program's by a relative error of at most 0.0095.
The reference program's roundings to bfloat16 on the way count: a program that leaves them out, or rounds other values in their place, can miss the bound.
Values may be sent and summed in bfloat16 or wider, within the bound.
A program may use at most 64 MiB of HBM per device.

```python
import math
import jax
import jax.numpy as jnp
import numpy as np
from jax import lax

D = 2048
HD = 128
HEADS = 16
KV = 2
FF = 4096
TOP = 2
GRID_W = 64
TOKENS = 2048
TOK_DEV = 64
EXPERTS = 8
CAP = 32
N_TP = 4


def shared_keys(key):
    base = jax.random.normal(jax.random.fold_in(key, 101), (TOKENS, KV * HD), jnp.float32)
    return jnp.clip(base, -6.0, 6.0)


def draw_keys(key, part):
    return shared_keys(key).astype(jnp.bfloat16)


def draw_queries(key, part):
    base = jax.random.normal(jax.random.fold_in(key, 202), (TOKENS, HEADS * HD), jnp.float32)
    base = jnp.clip(base, -6.0, 6.0)
    return base.astype(jnp.bfloat16)


def draw_query_gain(key, part):
    uniform_draw = jax.random.uniform(jax.random.fold_in(key, 303), (HD,), jnp.float32)
    return 0.1 + 1.8 * uniform_draw


def draw_key_gain(key, part):
    uniform_draw = jax.random.uniform(jax.random.fold_in(key, 404), (HD,), jnp.float32)
    return 0.1 + 1.8 * uniform_draw


def shard_levels(stream_key, dims, pieces, smallest, largest):
    def one(dim, blocks):
        heights = jax.random.uniform(jax.random.fold_in(jax.random.fold_in(stream_key, 6), dim), (blocks,), jnp.float32, smallest / len(pieces), largest / len(pieces))
        return jnp.repeat(jnp.exp(heights), dims[dim] // blocks).reshape((-1,) + (1,) * (len(dims) - dim - 1))

    level = one(*pieces[0])
    for cut in pieces[1:]:
        level = level * one(*cut)
    return level


def assign_block(own_key, own, number, rows, count, top, bound, skew):
    ranking = jax.random.permutation(own_key, count)
    packed, common = load_shares(count, rows * top, bound, skew, True), load_shares(count, rows * top, bound, skew, False)
    places = jnp.arange(count)

    def named(lengths, offset_by):
        used = int((lengths > 0).sum())
        fixed = max(1, used // 4)
        shifted = fixed + (places - fixed + offset_by * (used - fixed)) % max(1, count - fixed)
        return jnp.zeros((count,), jnp.int32).at[ranking[jnp.where(places < fixed, places, shifted)]].set(jnp.asarray(lengths, jnp.int32))

    lengths = jnp.where(number % 4 == 0, named(packed, number // 4), named(common, number - number // 4 - 1))
    mixed = jax.random.permutation(jax.random.fold_in(own, 3), count)
    source_of, taker = mixed[0:count // 2 * 2:2], mixed[1:count // 2 * 2:2]
    slack = jnp.minimum(lengths[source_of] - 1, bound - lengths[taker]) // 2
    slack = jnp.where((source_of == ranking[0]) | (taker == ranking[0]) | (lengths[taker] == 0), 0, jnp.maximum(slack, 0))
    shifted = jax.random.randint(jax.random.fold_in(own, 4), (count // 2,), 0, 1 << 20) % (slack + 1)
    lengths = lengths.at[source_of].add(-shifted).at[taker].add(shifted)
    labels = jnp.searchsorted(jnp.cumsum(lengths), jnp.arange(rows * top), side="right").astype(jnp.int32)
    grid = labels.reshape(top, rows).T
    grid = grid[jax.random.permutation(jax.random.fold_in(own, 1), rows)]
    offset_by = jax.random.randint(jax.random.fold_in(own, 2), (rows, 1), 0, top)
    return jnp.take_along_axis(grid, (jnp.arange(top)[None, :] + offset_by) % top, axis=1)


def load_shares(number_of, total, most, skew, full):
    weights = [(1 << 20) // math.isqrt(rank ** skew) + 1 for rank in range(1, number_of + 1)]
    largest = most if full else min(most, max(-(-total // number_of), total * weights[0] // sum(weights)))
    least = 1 if total - largest >= number_of - 1 else 0
    holding, rest = [largest] + [least] * (number_of - 1), total - largest - least * (number_of - 1)
    while rest > 0:
        candidates = [i for i in range(1, number_of) if holding[i] < largest] or [i for i in range(1, number_of) if holding[i] < most]
        mass, remaining = sum([weights[i] for i in candidates]), rest
        for i in candidates:
            extra = min(most - holding[i], max(1, remaining * weights[i] // mass), rest)
            holding[i] = holding[i] + extra
            rest = rest - extra
    return np.array(holding)


def centred(key, extent, scale, reach, split=(), held_as=jnp.bfloat16):
    result = scale * jax.random.normal(key, extent, jnp.float32)
    if split:
        result = result * shard_levels(key, extent, split, -0.22, 0.18)
    return jnp.clip(result, -reach, reach).astype(held_as)


def setup_inputs(seed: int = 0) -> dict:
    streams_of = jax.random.split(jax.random.key(seed), 14)
    queries = draw_queries(jax.random.fold_in(streams_of[13], 71), 0)
    keys = draw_keys(jax.random.fold_in(streams_of[13], 71), 0)
    values = centred(streams_of[2], (TOKENS, KV * HD), 1.0, 6.0, ((0, 8),))
    query_gain = draw_query_gain(jax.random.fold_in(streams_of[13], 71), 0)
    key_gain = draw_key_gain(jax.random.fold_in(streams_of[13], 71), 0)
    out_proj = centred(streams_of[5], (HEADS * HD, D), (HEADS * HD) ** -0.5, 0.125, ((1, 4),))
    expert_norm_scale = jnp.clip(1.0 + 0.18 * jax.random.normal(streams_of[6], (D,), jnp.float32), 0.1, 1.9)
    residual = centred(streams_of[7], (TOKENS, D), 1.0, 6.0, ((0, 32),))
    routes_keys = jax.random.split(jax.random.fold_in(streams_of[8], 1), TOKENS // TOK_DEV)
    routes_turns = jax.random.permutation(jax.random.fold_in(streams_of[8], 3), TOKENS // TOK_DEV)
    routes = jax.vmap(lambda own, number: assign_block(jax.random.fold_in(streams_of[8], 2), own, number, TOK_DEV, EXPERTS, TOP, CAP, 1))(routes_keys, routes_turns).reshape((TOKENS, TOP))
    route_weights = jnp.clip(0.1 + 0.79999997 * jax.random.uniform(streams_of[9], (TOKENS, TOP), jnp.float32) ** shard_levels(streams_of[9], (TOKENS, TOP), ((0, 32),), -0.2, 0.2), 0.1, 0.9)
    w_gate = centred(streams_of[10], (EXPERTS, D, FF), D ** -0.5, 0.125, ((0, 8), (2, 4)))
    w_up = centred(streams_of[11], (EXPERTS, D, FF), D ** -0.5, 0.125, ((0, 8), (2, 4)))
    w_down = centred(streams_of[12], (EXPERTS, FF, D), FF ** -0.5, 0.09375, ((0, 8), (1, 4)))
    return dict(queries=queries, keys=keys, values=values, query_gain=query_gain, key_gain=key_gain, out_proj=out_proj, expert_norm_scale=expert_norm_scale, residual=residual, routes=routes, route_weights=route_weights, w_gate=w_gate, w_up=w_up, w_down=w_down)


EPS = 1e-06
ROPE_BASE = 10000.0

def rotate(field, position):
    half = field.shape[-1] // 2
    quarter = half // 2
    freqs = ROPE_BASE ** (-jnp.arange(quarter, dtype=jnp.float32) / quarter)
    grid_row = (position // GRID_W).astype(jnp.float32)
    grid_col = (position % GRID_W).astype(jnp.float32)

    def turn_half(part, coord):
        angle = coord[:, None] * freqs[None, :]
        cosine = jnp.cos(angle)[:, None, :]
        sine = jnp.sin(angle)[:, None, :]
        first, second = (part[..., :quarter], part[..., quarter:])
        return jnp.concatenate([first * cosine - second * sine, second * cosine + first * sine], axis=-1)
    return jnp.concatenate([turn_half(field[..., :half], grid_row), turn_half(field[..., half:], grid_col)], axis=-1)

def prepare(field, gain, position):
    count = field.shape[0]
    width = gain.shape[0]
    heads_here = field.shape[1] // width
    values_f = field.reshape(count, heads_here, width).astype(jnp.float32)
    scaled = values_f * lax.rsqrt(lax.optimization_barrier(jnp.mean(values_f * values_f, axis=-1, keepdims=True)) + EPS) * gain
    return rotate(scaled, position).reshape(count, heads_here * width).astype(jnp.bfloat16)

def reference(queries, keys, values, query_gain, key_gain, out_proj, expert_norm_scale, residual, routes, route_weights, w_gate, w_up, w_down):
    position = jnp.arange(TOKENS, dtype=jnp.int32)
    q_rot = prepare(queries, query_gain, position)
    k_rot = prepare(keys, key_gain, position)
    group = HEADS // KV
    block = math.gcd(TOKENS, 1024)

    def one_head(head):
        shared_value_head = head // group
        query_cols = lax.dynamic_slice_in_dim(q_rot, (head * HD).astype(jnp.int32), HD, 1)
        key_cols = lax.dynamic_slice_in_dim(k_rot, (shared_value_head * HD).astype(jnp.int32), HD, 1)
        value_cols = lax.dynamic_slice_in_dim(values, (shared_value_head * HD).astype(jnp.int32), HD, 1)

        def attend(query_block):
            scores = jnp.dot(query_block, key_cols.T, preferred_element_type=jnp.float32) * HD ** (-0.5)
            row_max = lax.optimization_barrier(jnp.max(scores, axis=-1, keepdims=True))
            weight_tensors = jnp.exp(scores - row_max).astype(jnp.bfloat16)
            total = lax.optimization_barrier(jnp.sum(lax.optimization_barrier(weight_tensors).astype(jnp.float32), axis=-1, keepdims=True))
            summed = jnp.dot(weight_tensors, value_cols, preferred_element_type=jnp.float32)
            return (summed / total).astype(jnp.bfloat16)
        blocks = query_cols.reshape(TOKENS // block, block, HD)
        return lax.map(attend, blocks).reshape(TOKENS, HD)
    per_head = lax.map(one_head, jnp.arange(HEADS, dtype=jnp.int32))
    attn = per_head.transpose(1, 0, 2).reshape(TOKENS, HEADS * HD)
    projected = jnp.dot(attn, out_proj, preferred_element_type=jnp.float32).astype(jnp.bfloat16)
    mixed = (residual.astype(jnp.float32) + projected.astype(jnp.float32)).astype(jnp.bfloat16)
    mixed_float_output = mixed.astype(jnp.float32)
    normed = (mixed_float_output * lax.rsqrt(lax.optimization_barrier(jnp.mean(mixed_float_output * mixed_float_output, axis=-1, keepdims=True)) + EPS) * expert_norm_scale).astype(jnp.bfloat16)
    flat_routes = routes.reshape(-1)
    flat_weights = route_weights.reshape(-1)
    flat_token = jnp.arange(TOKENS * TOP, dtype=jnp.int32) // TOP
    most_rows = TOKENS // TOK_DEV * CAP
    block_ff = FF // N_TP

    def expert_step(totals, expert):
        order = jnp.argsort((flat_routes != expert).astype(jnp.int32), stable=True)[:most_rows].astype(jnp.int32)
        valid = flat_routes[order] == expert
        rows = normed[flat_token[order]]
        gate = jnp.dot(rows, w_gate[expert], preferred_element_type=jnp.float32)
        upper = jnp.dot(rows, w_up[expert], preferred_element_type=jnp.float32)
        hidden = (jax.nn.silu(gate) * upper).astype(jnp.bfloat16)
        hidden_blocks = hidden.reshape(most_rows, N_TP, block_ff).astype(jnp.float32)
        down_blocks = w_down[expert].reshape(N_TP, block_ff, D).astype(jnp.float32)
        partial_value = jnp.einsum('mjf,jfd->jmd', hidden_blocks, down_blocks).astype(jnp.bfloat16)
        summed = lax.optimization_barrier(jnp.sum(lax.optimization_barrier(partial_value).astype(jnp.float32), axis=0))
        expert_out = summed.astype(jnp.bfloat16)
        weighted = lax.optimization_barrier(expert_out).astype(jnp.float32) * flat_weights[order][:, None]
        weighted = jnp.where(valid[:, None], weighted, jnp.float32(0.0))
        return (totals.at[order].add(weighted), None)
    start = jnp.zeros((TOKENS * TOP, D), jnp.float32)
    totals, unused = lax.scan(expert_step, start, jnp.arange(EXPERTS, dtype=jnp.int32))
    moe_sum = lax.optimization_barrier(jnp.sum(totals.reshape(TOKENS, TOP, D), axis=1))
    return (mixed_float_output + moe_sum).astype(jnp.bfloat16)
```

```python
import functools

import jax
import jax.numpy as jnp
from jax import lax
from jax.experimental import pallas as pl
from jax.experimental.pallas import tpu as pltpu
from jax.sharding import PartitionSpec as P

GRID_W = 64


EPS = 1e-06
ROPE_BASE = 10000.0
NEG_START = -1e30


def rotate(field, position):
    half = field.shape[-1] // 2
    quarter = half // 2
    freqs = ROPE_BASE ** (-jnp.arange(quarter, dtype=jnp.float32) / quarter)
    grid_row = (position // GRID_W).astype(jnp.float32)
    grid_col = (position % GRID_W).astype(jnp.float32)

    def turn_half(part, coord):
        angle = coord[:, None] * freqs[None, :]
        cosine = jnp.cos(angle)[:, None, :]
        sine = jnp.sin(angle)[:, None, :]
        first, second = (part[..., :quarter], part[..., quarter:])
        return jnp.concatenate(
            [first * cosine - second * sine, second * cosine + first * sine], axis=-1
        )

    return jnp.concatenate(
        [turn_half(field[..., :half], grid_row), turn_half(field[..., half:], grid_col)], axis=-1
    )


def prepare(field, gain, position):
    count = field.shape[0]
    width = gain.shape[0]
    heads_here = field.shape[1] // width
    values_f = field.reshape(count, heads_here, width).astype(jnp.float32)
    scaled = (
        values_f * lax.rsqrt(jnp.mean(values_f * values_f, axis=-1, keepdims=True) + EPS) * gain
    )
    return rotate(scaled, position).reshape(count, heads_here * width).astype(jnp.bfloat16)


def absorb(carry, query_matrix, key_rows, value_rows, scale):
    count = key_rows.shape[0]
    width = 2048 if count > 2048 and count % 2048 == 0 else count
    key_blocks = key_rows.reshape(count // width, width, key_rows.shape[1], key_rows.shape[2])
    value_blocks = value_rows.reshape(
        count // width, width, value_rows.shape[1], value_rows.shape[2]
    )

    def step(state, block):
        run_max, run_sum, run_acc = state
        key_tile_rows, value_tile_rows = block
        scores = (
            jnp.einsum(
                "hxt,ght->hxg", query_matrix, key_tile_rows, preferred_element_type=jnp.float32
            )
            * scale
        )
        new_max = jnp.maximum(run_max, jnp.max(scores, axis=-1))
        weight_tensors = jnp.exp(scores - new_max[..., None]).astype(jnp.bfloat16)
        factor = jnp.exp(run_max - new_max)
        run_sum = run_sum * factor + jnp.sum(weight_tensors.astype(jnp.float32), axis=-1)
        run_acc = run_acc * factor[..., None] + jnp.einsum(
            "zij,jzu->ziu", weight_tensors, value_tile_rows, preferred_element_type=jnp.float32
        )
        return ((new_max, run_sum, run_acc), None)

    result, unused = lax.scan(step, carry, (key_blocks, value_blocks))
    return result


MESH = pl.DeviceIdType.MESH
VMEM_LIMIT = 60 * 1024 * 1024


def greet(partners, count):
    barrier = pltpu.get_barrier_semaphore()
    for where in partners:
        pl.semaphore_signal(barrier, inc=1, device_id=where, device_id_type=MESH)
    pl.semaphore_wait(barrier, count)


def remote(src, dst, send, recv, where):
    return pltpu.make_async_remote_copy(
        src_ref=src, dst_ref=dst, send_sem=send, recv_sem=recv, device_id=where, device_id_type=MESH
    )


def square():
    mine = lax.axis_index("tp")
    return mine, mine + 1 - 2 * lax.rem(mine, 2), lax.rem(mine + 2, 4), 3 - mine


def gather_kernel(n, k_ref, v_ref, ko_ref, vo_ref, send, recv):
    me = lax.axis_index("sp")
    chips = n // 2
    chip, core = me // 2, lax.rem(me, 2)
    partner = 2 * chip + 1 - core
    rows = k_ref.shape[0]
    has_right, has_left = chip < chips - 1, chip > 0
    right, left = me + 2, me - 2
    barrier = pltpu.get_barrier_semaphore()
    pl.semaphore_signal(barrier, inc=1, device_id={"sp": partner}, device_id_type=MESH)

    @pl.when(has_right)
    def _():
        pl.semaphore_signal(barrier, inc=1, device_id={"sp": right}, device_id_type=MESH)

    @pl.when(has_left)
    def _():
        pl.semaphore_signal(barrier, inc=1, device_id={"sp": left}, device_id_type=MESH)

    pl.semaphore_wait(barrier, 1 + has_right.astype(jnp.int32) + has_left.astype(jnp.int32))

    def block(out, origin):
        return out.at[pl.ds(pl.multiple_of(origin * rows, rows), rows)]

    def copies(origin, way, where, own=False):
        return [
            remote(
                ref if own else block(out, origin),
                block(out, origin),
                send.at[origin, way, i],
                recv.at[origin, i],
                {"sp": where},
            )
            for i, (ref, out) in enumerate(((k_ref, ko_ref), (v_ref, vo_ref)))
        ]

    def start(*args, **kw):
        for c in copies(*args, **kw):
            c.start()

    def sent(*args, **kw):
        for c in copies(*args, **kw):
            c.wait_send()

    def arrived(origin):
        for c in copies(origin, 0, partner):
            c.wait_recv()

    @pl.when(has_right)
    def _():
        start(me, 0, right, own=True)

    @pl.when(has_left)
    def _():
        start(me, 2, left, own=True)

    start(me, 1, partner, own=True)
    block(ko_ref, me)[...] = k_ref[...]
    block(vo_ref, me)[...] = v_ref[...]
    for j in range(1, chips):

        @pl.when(chip - j >= 0)
        def _(origin=me - 2 * j):
            arrived(origin)

            @pl.when(has_right)
            def _():
                start(origin, 0, right)

            start(origin, 1, partner)

        @pl.when(chip + j < chips)
        def _(origin=me + 2 * j):
            arrived(origin)

            @pl.when(has_left)
            def _():
                start(origin, 2, left)

            start(origin, 1, partner)

    for z in range(chips):
        arrived(2 * z + 1 - core)
    sent(me, 1, partner, own=True)

    @pl.when(has_right)
    def _():
        sent(me, 0, right, own=True)

    @pl.when(has_left)
    def _():
        sent(me, 2, left, own=True)

    for j in range(1, chips):

        @pl.when(chip - j >= 0)
        def _(origin=me - 2 * j):
            @pl.when(has_right)
            def _():
                sent(origin, 0, right)

            sent(origin, 1, partner)

        @pl.when(chip + j < chips)
        def _(origin=me + 2 * j):
            @pl.when(has_left)
            def _():
                sent(origin, 2, left)

            sent(origin, 1, partner)


def in_vmem(count):
    return [pl.BlockSpec(memory_space=pltpu.VMEM)] * count


def params(number):
    return pltpu.CompilerParams(
        collective_id=number, has_side_effects=True, vmem_limit_bytes=VMEM_LIMIT
    )


def gather_rows(n, own_keys, own_values):
    rows, width = own_keys.shape
    shape = jax.ShapeDtypeStruct((n * rows, width), own_keys.dtype)
    return pl.pallas_call(
        functools.partial(gather_kernel, n),
        out_shape=(shape, shape),
        in_specs=in_vmem(2),
        out_specs=tuple(in_vmem(2)),
        scratch_shapes=[pltpu.SemaphoreType.DMA((n, 3, 2)), pltpu.SemaphoreType.DMA((n, 2))],
        compiler_params=params(0),
        name="gather_rows",
    )(own_keys, own_values)


def project_kernel(attn_ref, w_ref, out_ref, held, stage, send, recv, give, take):
    mine, across, along, corner = square()
    rows, width = attn_ref.shape
    half = rows // 2
    share = out_ref.shape[0]
    greet([{"tp": across}, {"tp": along}, {"tp": corner}], 3)
    first = [
        remote(attn_ref, held.at[mine], send.at[0], recv.at[0], {"tp": across}),
        remote(attn_ref, held.at[mine], send.at[1], recv.at[1], {"tp": along}),
    ]
    for c in first:
        c.start()
    top, low = pl.ds(0, half), pl.ds(half, half)
    second = [
        remote(held.at[across, top], held.at[across, top], send.at[2], recv.at[2], {"tp": along}),
        remote(held.at[along, low], held.at[along, low], send.at[3], recv.at[3], {"tp": across}),
    ]

    def term(rows_here, owner):
        part = w_ref[pl.ds(pl.multiple_of(owner * width, width), width), :]
        return jnp.dot(rows_here, part, preferred_element_type=jnp.float32)

    total = term(attn_ref[...], mine)
    first[0].wait_recv()
    second[0].start()
    first[1].wait_recv()
    second[1].start()
    total += term(held[across], across)
    total += term(held[along], along)
    for c in second:
        c.wait_recv()
    total += term(held[corner], corner)
    stage[...] = total.astype(stage.dtype)
    columns = pl.ds(pl.multiple_of(mine * width, width), width)

    def piece(owner):
        return pl.ds(pl.multiple_of(owner * share, share), share)

    back = [
        remote(stage.at[piece(p)], out_ref.at[:, columns], give.at[i], take.at[i], {"tp": p})
        for i, p in enumerate((corner, across, along))
    ]
    for c in back:
        c.start()
    out_ref[:, columns] = stage[piece(mine), :]
    for c in back:
        c.wait()
    for c in first + second:
        c.wait_send()


def project(attn, out_proj, share):
    rows, width = attn.shape
    parts = out_proj.shape[0] // width
    return pl.pallas_call(
        project_kernel,
        out_shape=jax.ShapeDtypeStruct((share, out_proj.shape[1] * parts), jnp.bfloat16),
        in_specs=in_vmem(2),
        out_specs=in_vmem(1)[0],
        scratch_shapes=[
            pltpu.VMEM((parts, rows, width), jnp.bfloat16),
            pltpu.VMEM((rows, out_proj.shape[1]), jnp.bfloat16),
            pltpu.SemaphoreType.DMA((4,)),
            pltpu.SemaphoreType.DMA((4,)),
            pltpu.SemaphoreType.DMA((3,)),
            pltpu.SemaphoreType.DMA((3,)),
        ],
        compiler_params=params(1),
        name="project",
    )(attn, out_proj)


def everyone(n, me):
    mine, across, along, corner = square()
    peers = [{"sp": lax.rem(me + off, n)} for off in range(1, n)]
    return peers + [{"tp": across}, {"tp": along}]


def dispatch_kernel(n, chunks, rows_ref, out_ref, own_sem, send, recv, send_sq, recv_sq):
    me = lax.axis_index("sp")
    mine, across, along, corner = square()
    width = rows_ref.shape[-1] // chunks
    greet(everyone(n, me), n + 1)
    own = pltpu.make_async_copy(rows_ref.at[me], out_ref.at[mine, me], own_sem)
    own.start()

    def columns(k):
        return pl.ds(k * width, width)

    def scatter(k, off):
        to = lax.rem(me + off, n)
        return remote(
            rows_ref.at[to, :, columns(k)],
            out_ref.at[mine, me, :, columns(k)],
            send.at[k, off],
            recv.at[k, off],
            {"sp": to},
        )

    for k in range(chunks):
        for off in range(1, n):
            scatter(k, off).start()
    own.wait()

    def pass_on(k, way):
        half = width // 2
        group, cols, where = (
            (mine, columns(k), across),
            (mine, columns(k), along),
            (across, pl.ds(k * width, half), along),
            (along, pl.ds(k * width + half, half), across),
        )[way]
        ref = out_ref.at[group, :, :, cols]
        return remote(ref, ref, send_sq.at[k, way], recv_sq.at[k, way], {"tp": where})

    def forward(k):
        for way in (0, 1):
            pass_on(k, way).wait_recv()
            pass_on(k, way + 2).start()

    for k in range(chunks):
        for off in range(1, n):
            scatter(k, off).wait_recv()
        pass_on(k, 0).start()
        pass_on(k, 1).start()
        if k:
            forward(k - 1)
    forward(chunks - 1)
    for k in range(chunks):
        for way in (2, 3):
            pass_on(k, way).wait_recv()
    for k in range(chunks):
        for off in range(1, n):
            scatter(k, off).wait_send()
        for way in range(4):
            pass_on(k, way).wait_send()


def dispatch(n, parts, rows, chunks=4):
    count, capacity, width = rows.shape
    return pl.pallas_call(
        functools.partial(dispatch_kernel, n, chunks),
        out_shape=jax.ShapeDtypeStruct((parts, count, capacity, width), rows.dtype),
        in_specs=in_vmem(1),
        out_specs=pl.BlockSpec(memory_space=pl.ANY),
        scratch_shapes=[
            pltpu.SemaphoreType.DMA,
            pltpu.SemaphoreType.DMA((chunks, n)),
            pltpu.SemaphoreType.DMA((chunks, n)),
            pltpu.SemaphoreType.DMA((chunks, 4)),
            pltpu.SemaphoreType.DMA((chunks, 4)),
        ],
        compiler_params=params(2),
        name="dispatch",
    )(rows)


def combine_kernel(
    n, chunks, y_ref, out_ref, from_x, from_y, to_y, to_x, last_x, last_y, done, send, recv, send_sq, recv_sq
):
    me = lax.axis_index("sp")
    mine, across, along, corner = square()
    x, y = lax.rem(mine, 2), mine // 2
    capacity = out_ref.shape[1]
    half = out_ref.shape[2] // chunks // 2
    greet(everyone(n, me), n + 1)

    def cols(k, side):
        return pl.ds((2 * k + side) * half, half)

    def hop(k, way):
        src, dst, where = (
            (y_ref.at[:, 1 - x, :, cols(k, 0)], from_x.at[k], across),
            (y_ref.at[1 - y, :, :, cols(k, 1)], from_y.at[k], along),
            (to_y.at[k], last_y.at[k], along),
            (to_x.at[k], last_x.at[k], across),
        )[way]
        return remote(src, dst, send_sq.at[k, way], recv_sq.at[k, way], {"tp": where})

    def home(k, off):
        to = lax.rem(me + off, n)
        return remote(
            done.at[k, to],
            out_ref.at[me, :, pl.ds(2 * k * half, 2 * half)],
            send.at[k, off],
            recv.at[k, off],
            {"sp": to},
        )

    for k in range(chunks):
        hop(k, 0).start()
        hop(k, 1).start()

    def wide(value):
        return value.astype(jnp.float32)

    def finish(k):
        hop(k, 2).wait_recv()
        low = wide(y_ref[y, x, :, cols(k, 0)]) + wide(from_x[k, y]) + wide(last_y[k])
        done[k, :, :, pl.ds(0, half)] = low.astype(done.dtype).reshape(n, capacity, half)
        hop(k, 3).wait_recv()
        high = wide(y_ref[y, x, :, cols(k, 1)]) + wide(from_y[k, x]) + wide(last_x[k])
        done[k, :, :, pl.ds(half, half)] = high.astype(done.dtype).reshape(n, capacity, half)
        for off in range(1, n):
            home(k, off).start()
        out_ref[me, :, pl.ds(2 * k * half, 2 * half)] = done[k, me]

    for k in range(chunks):
        hop(k, 0).wait_recv()
        to_y[k] = (wide(y_ref[1 - y, x, :, cols(k, 0)]) + wide(from_x[k, 1 - y])).astype(to_y.dtype)
        hop(k, 2).start()
        hop(k, 1).wait_recv()
        to_x[k] = (wide(y_ref[y, 1 - x, :, cols(k, 1)]) + wide(from_y[k, 1 - x])).astype(to_x.dtype)
        hop(k, 3).start()
        if k:
            finish(k - 1)
    finish(chunks - 1)
    for k in range(chunks):
        for off in range(1, n):
            home(k, off).wait()
        for way in range(4):
            hop(k, way).wait_send()


def combine(n, partial, capacity, chunks=4):
    rows, width = partial.shape[2:]
    half = width // chunks // 2
    one = pltpu.VMEM((chunks, rows, half), partial.dtype)
    two = pltpu.VMEM((chunks, 2, rows, half), partial.dtype)
    return pl.pallas_call(
        functools.partial(combine_kernel, n, chunks),
        out_shape=jax.ShapeDtypeStruct((n, capacity, width), partial.dtype),
        in_specs=in_vmem(1),
        out_specs=in_vmem(1)[0],
        scratch_shapes=[
            two,
            two,
            one,
            one,
            one,
            one,
            pltpu.VMEM((chunks, n, capacity, 2 * half), partial.dtype),
            pltpu.SemaphoreType.DMA((chunks, n)),
            pltpu.SemaphoreType.DMA((chunks, n)),
            pltpu.SemaphoreType.DMA((chunks, 4)),
            pltpu.SemaphoreType.DMA((chunks, 4)),
        ],
        compiler_params=params(3),
        name="combine",
    )(partial)


def start_state(batch, rows, width):
    return (
        jnp.full((batch, rows), NEG_START, jnp.float32),
        jnp.zeros((batch, rows), jnp.float32),
        jnp.zeros((batch, rows, width), jnp.float32),
    )


def local(
    queries,
    keys,
    values,
    query_gain,
    key_gain,
    out_proj,
    expert_norm_scale,
    residual,
    routes,
    route_weights,
    w_gate,
    w_up,
    w_down,
):
    head_size = query_gain.shape[0]
    tok_sp = queries.shape[0]
    tp_count = lax.axis_size("tp")
    sp_count = lax.axis_size("sp")
    heads_dev = queries.shape[1] // head_size
    all_heads = heads_dev * tp_count
    kv_heads = keys.shape[1] // head_size
    group = all_heads // kv_heads
    scale = head_size ** (-0.5)
    tp_index = lax.axis_index("tp")
    sp_index = lax.axis_index("sp")
    position = sp_index * tok_sp + jnp.arange(tok_sp, dtype=jnp.int32)
    q_rot = prepare(queries, query_gain, position)
    shared_value_head = tp_index * heads_dev // group
    own_keys = prepare(
        lax.dynamic_slice_in_dim(keys, shared_value_head * head_size, head_size, 1),
        key_gain,
        position,
    )
    own_values = lax.dynamic_slice_in_dim(values, shared_value_head * head_size, head_size, 1)
    query_matrix = (
        q_rot.reshape(tok_sp, heads_dev, head_size)
        .transpose(1, 0, 2)
        .reshape(1, heads_dev * tok_sp, head_size)
    )
    tok_dev = residual.shape[0]
    top = routes.shape[1]
    capacity = max(2, 2 * tok_dev * top // sp_count)
    direct = tp_count == 4 and sp_count % 2 == 0 and capacity % 16 == 0
    if direct:
        key_piece, value_piece = gather_rows(sp_count, own_keys, own_values)
    else:
        key_piece = lax.all_gather(own_keys, "sp", axis=0, tiled=True)
        value_piece = lax.all_gather(own_values, "sp", axis=0, tiled=True)
    run_max, run_sum, run_acc = absorb(
        start_state(1, heads_dev * tok_sp, head_size),
        query_matrix,
        key_piece[:, None, :],
        value_piece[:, None, :],
        scale,
    )
    attn = (run_acc / run_sum[..., None]).astype(jnp.bfloat16)
    attn = (
        attn.reshape(heads_dev, tok_sp, head_size)
        .transpose(1, 0, 2)
        .reshape(tok_sp, heads_dev * head_size)
    )
    if direct:
        projected = project(attn, out_proj, tok_dev)
    else:
        columns = jnp.dot(
            lax.all_gather(attn, "tp", axis=1, tiled=True),
            out_proj,
            preferred_element_type=jnp.float32,
        )
        projected = lax.all_to_all(
            columns.astype(jnp.bfloat16), "tp", split_axis=0, concat_axis=1, tiled=True
        )
    mixed_float_output = residual.astype(jnp.float32) + projected.astype(jnp.float32)
    mixed = mixed_float_output.astype(jnp.bfloat16)
    mixed_float_output = mixed.astype(jnp.float32)
    normed = (
        mixed_float_output
        * lax.rsqrt(jnp.mean(mixed_float_output * mixed_float_output, axis=-1, keepdims=True) + EPS)
        * expert_norm_scale
    ).astype(jnp.bfloat16)
    flat_routes = routes.reshape(-1)
    one_hot = (flat_routes[:, None] == jnp.arange(sp_count, dtype=jnp.int32)[None, :]).astype(
        jnp.int32
    )
    earlier = jnp.cumsum(one_hot, axis=0) - one_hot
    slot_index = jnp.sum(earlier * one_hot, axis=1)
    target = flat_routes * capacity + slot_index
    selector = (
        jnp.arange(sp_count * capacity, dtype=jnp.int32)[:, None] == target[None, :]
    ).astype(jnp.bfloat16)
    selector = jnp.sum(selector.reshape(sp_count * capacity, tok_dev, top), axis=2)
    send_rows = jnp.dot(selector, normed, preferred_element_type=jnp.float32).astype(jnp.bfloat16)
    gate_weight = w_gate[0]
    up_weight = w_up[0]
    down_weight = w_down[0]
    if direct:
        piece = dispatch(
            sp_count, tp_count, send_rows.reshape(sp_count, capacity, send_rows.shape[1])
        ).reshape(tp_count * sp_count * capacity, send_rows.shape[1])
    else:
        arrived = lax.all_to_all(send_rows, "sp", split_axis=0, concat_axis=0, tiled=True)
        piece = lax.all_gather(arrived, "tp", axis=0, tiled=True)
    gate = jnp.dot(piece, gate_weight, preferred_element_type=jnp.float32)
    upper = jnp.dot(piece, up_weight, preferred_element_type=jnp.float32)
    hidden = (jax.nn.silu(gate) * upper).astype(jnp.bfloat16)
    partial = jnp.dot(hidden, down_weight, preferred_element_type=jnp.float32).astype(jnp.bfloat16)
    if direct:
        width = partial.shape[1]
        returned = combine(
            sp_count, partial.reshape(2, 2, sp_count * capacity, width), capacity
        ).reshape(sp_count * capacity, width)
    else:
        expert_out = lax.psum_scatter(partial, "tp", scatter_dimension=0, tiled=True)
        returned = lax.all_to_all(expert_out, "sp", split_axis=0, concat_axis=0, tiled=True)
    picked = (
        jnp.take(returned, target, axis=0)
        .astype(jnp.float32)
        .reshape(tok_dev, top, returned.shape[1])
    )
    moe_sum = jnp.sum(picked * route_weights[:, :, None], axis=1)
    return (mixed_float_output + moe_sum).astype(jnp.bfloat16)


def solution(mesh):
    placed = (
        P("sp", "tp"),
        P("sp", None),
        P("sp", None),
        P(),
        P(),
        P(None, "tp"),
        P(),
        P(("sp", "tp"), None),
        P(("sp", "tp"), None),
        P(("sp", "tp"), None),
        P("sp", None, "tp"),
        P("sp", None, "tp"),
        P("sp", "tp", None),
    )
    return jax.shard_map(
        local, mesh=mesh, in_specs=placed, out_specs=P(("sp", "tp"), None), check_vma=False
    )
```

```python
import functools

import jax
import jax.numpy as jnp
from jax import lax
from jax.experimental import pallas as pl
from jax.experimental.pallas import tpu as pltpu
from jax.sharding import PartitionSpec as P

GRID_W = 64


EPS = 1e-06
ROPE_BASE = 10000.0
NEG_START = -1e30


def rotate(field, position):
    half = field.shape[-1] // 2
    quarter = half // 2
    freqs = ROPE_BASE ** (-jnp.arange(quarter, dtype=jnp.float32) / quarter)
    grid_row = (position // GRID_W).astype(jnp.float32)
    grid_col = (position % GRID_W).astype(jnp.float32)

    def turn_half(part, coord):
        angle = coord[:, None] * freqs[None, :]
        cosine = jnp.cos(angle)[:, None, :]
        sine = jnp.sin(angle)[:, None, :]
        first, second = (part[..., :quarter], part[..., quarter:])
        return jnp.concatenate(
            [first * cosine - second * sine, second * cosine + first * sine], axis=-1
        )

    return jnp.concatenate(
        [turn_half(field[..., :half], grid_row), turn_half(field[..., half:], grid_col)], axis=-1
    )


def prepare(field, gain, position):
    count = field.shape[0]
    width = gain.shape[0]
    heads_here = field.shape[1] // width
    values_f = field.reshape(count, heads_here, width).astype(jnp.float32)
    scaled = (
        values_f * lax.rsqrt(jnp.mean(values_f * values_f, axis=-1, keepdims=True) + EPS) * gain
    )
    return rotate(scaled, position).reshape(count, heads_here * width).astype(jnp.bfloat16)


def absorb(carry, query_matrix, key_rows, value_rows, scale):
    count = key_rows.shape[0]
    width = 2048 if count > 2048 and count % 2048 == 0 else count
    key_blocks = key_rows.reshape(count // width, width, key_rows.shape[1], key_rows.shape[2])
    value_blocks = value_rows.reshape(
        count // width, width, value_rows.shape[1], value_rows.shape[2]
    )

    def step(state, block):
        run_max, run_sum, run_acc = state
        key_tile_rows, value_tile_rows = block
        scores = (
            jnp.einsum(
                "hxt,ght->hxg", query_matrix, key_tile_rows, preferred_element_type=jnp.float32
            )
            * scale
        )
        new_max = jnp.maximum(run_max, jnp.max(scores, axis=-1))
        weight_tensors = jnp.exp(scores - new_max[..., None]).astype(jnp.bfloat16)
        factor = jnp.exp(run_max - new_max)
        run_sum = run_sum * factor + jnp.sum(weight_tensors.astype(jnp.float32), axis=-1)
        run_acc = run_acc * factor[..., None] + jnp.einsum(
            "zij,jzu->ziu", weight_tensors, value_tile_rows, preferred_element_type=jnp.float32
        )
        return ((new_max, run_sum, run_acc), None)

    result, unused = lax.scan(step, carry, (key_blocks, value_blocks))
    return result


MESH = pl.DeviceIdType.MESH
VMEM_LIMIT = 60 * 1024 * 1024


def greet(partners, count):
    barrier = pltpu.get_barrier_semaphore()
    for where in partners:
        pl.semaphore_signal(barrier, inc=1, device_id=where, device_id_type=MESH)
    pl.semaphore_wait(barrier, count)


def remote(src, dst, send, recv, where):
    return pltpu.make_async_remote_copy(
        src_ref=src, dst_ref=dst, send_sem=send, recv_sem=recv, device_id=where, device_id_type=MESH
    )


def square():
    mine = lax.axis_index("tp")
    return mine, mine + 1 - 2 * lax.rem(mine, 2), lax.rem(mine + 2, 4), 3 - mine


def gather_kernel(n, k_ref, v_ref, ko_ref, vo_ref, send, recv):
    me = lax.axis_index("sp")
    chips = n // 2
    chip, core = me // 2, lax.rem(me, 2)
    partner = 2 * chip + 1 - core
    rows = k_ref.shape[0]
    has_right, has_left = chip < chips - 1, chip > 0
    right, left = me + 2, me - 2
    barrier = pltpu.get_barrier_semaphore()
    pl.semaphore_signal(barrier, inc=1, device_id={"sp": partner}, device_id_type=MESH)

    @pl.when(has_right)
    def _():
        pl.semaphore_signal(barrier, inc=1, device_id={"sp": right}, device_id_type=MESH)

    @pl.when(has_left)
    def _():
        pl.semaphore_signal(barrier, inc=1, device_id={"sp": left}, device_id_type=MESH)

    pl.semaphore_wait(barrier, 1 + has_right.astype(jnp.int32) + has_left.astype(jnp.int32))

    def block(out, origin):
        return out.at[pl.ds(pl.multiple_of(origin * rows, rows), rows)]

    def copies(origin, way, where, own=False):
        return [
            remote(
                ref if own else block(out, origin),
                block(out, origin),
                send.at[origin, way, i],
                recv.at[origin, i],
                {"sp": where},
            )
            for i, (ref, out) in enumerate(((k_ref, ko_ref), (v_ref, vo_ref)))
        ]

    def start(*args, **kw):
        for c in copies(*args, **kw):
            c.start()

    def sent(*args, **kw):
        for c in copies(*args, **kw):
            c.wait_send()

    def arrived(origin):
        for c in copies(origin, 0, partner):
            c.wait_recv()

    @pl.when(has_right)
    def _():
        start(me, 0, right, own=True)

    @pl.when(has_left)
    def _():
        start(me, 2, left, own=True)

    start(me, 1, partner, own=True)
    block(ko_ref, me)[...] = k_ref[...]
    block(vo_ref, me)[...] = v_ref[...]
    for j in range(1, chips):

        @pl.when(chip - j >= 0)
        def _(origin=me - 2 * j):
            arrived(origin)

            @pl.when(has_right)
            def _():
                start(origin, 0, right)

            start(origin, 1, partner)

        @pl.when(chip + j < chips)
        def _(origin=me + 2 * j):
            arrived(origin)

            @pl.when(has_left)
            def _():
                start(origin, 2, left)

            start(origin, 1, partner)

    for z in range(chips):
        arrived(2 * z + 1 - core)
    sent(me, 1, partner, own=True)

    @pl.when(has_right)
    def _():
        sent(me, 0, right, own=True)

    @pl.when(has_left)
    def _():
        sent(me, 2, left, own=True)

    for j in range(1, chips):

        @pl.when(chip - j >= 0)
        def _(origin=me - 2 * j):
            @pl.when(has_right)
            def _():
                sent(origin, 0, right)

            sent(origin, 1, partner)

        @pl.when(chip + j < chips)
        def _(origin=me + 2 * j):
            @pl.when(has_left)
            def _():
                sent(origin, 2, left)

            sent(origin, 1, partner)


def in_vmem(count):
    return [pl.BlockSpec(memory_space=pltpu.VMEM)] * count


def params(number):
    return pltpu.CompilerParams(
        collective_id=number, has_side_effects=True, vmem_limit_bytes=VMEM_LIMIT
    )


def gather_rows(n, own_keys, own_values):
    rows, width = own_keys.shape
    shape = jax.ShapeDtypeStruct((n * rows, width), own_keys.dtype)
    return pl.pallas_call(
        functools.partial(gather_kernel, n),
        out_shape=(shape, shape),
        in_specs=in_vmem(2),
        out_specs=tuple(in_vmem(2)),
        scratch_shapes=[pltpu.SemaphoreType.DMA((n, 3, 2)), pltpu.SemaphoreType.DMA((n, 2))],
        compiler_params=params(0),
        name="gather_rows",
    )(own_keys, own_values)


def project_kernel(attn_ref, w_ref, out_ref, held, stage, send, recv, give, take):
    mine, across, along, corner = square()
    rows, width = attn_ref.shape
    half = rows // 2
    share = out_ref.shape[0]
    greet([{"tp": across}, {"tp": along}, {"tp": corner}], 3)
    first = [
        remote(attn_ref, held.at[mine], send.at[0], recv.at[0], {"tp": across}),
        remote(attn_ref, held.at[mine], send.at[1], recv.at[1], {"tp": along}),
    ]
    for c in first:
        c.start()
    top, low = pl.ds(0, half), pl.ds(half, half)
    second = [
        remote(held.at[across, top], held.at[across, top], send.at[2], recv.at[2], {"tp": along}),
        remote(held.at[along, low], held.at[along, low], send.at[3], recv.at[3], {"tp": across}),
    ]

    def term(rows_here, owner):
        part = w_ref[pl.ds(pl.multiple_of(owner * width, width), width), :]
        return jnp.dot(rows_here, part, preferred_element_type=jnp.float32)

    total = term(attn_ref[...], mine)
    first[0].wait_recv()
    second[0].start()
    first[1].wait_recv()
    second[1].start()
    total += term(held[across], across)
    total += term(held[along], along)
    for c in second:
        c.wait_recv()
    total += term(held[corner], corner)
    stage[...] = total.astype(stage.dtype)
    columns = pl.ds(pl.multiple_of(mine * width, width), width)

    def piece(owner):
        return pl.ds(pl.multiple_of(owner * share, share), share)

    back = [
        remote(stage.at[piece(p)], out_ref.at[:, columns], give.at[i], take.at[i], {"tp": p})
        for i, p in enumerate((corner, across, along))
    ]
    for c in back:
        c.start()
    out_ref[:, columns] = stage[piece(mine), :]
    for c in back:
        c.wait()
    for c in first + second:
        c.wait_send()


def project(attn, out_proj, share):
    rows, width = attn.shape
    parts = out_proj.shape[0] // width
    return pl.pallas_call(
        project_kernel,
        out_shape=jax.ShapeDtypeStruct((share, out_proj.shape[1] * parts), jnp.bfloat16),
        in_specs=in_vmem(2),
        out_specs=in_vmem(1)[0],
        scratch_shapes=[
            pltpu.VMEM((parts, rows, width), jnp.bfloat16),
            pltpu.VMEM((rows, out_proj.shape[1]), jnp.bfloat16),
            pltpu.SemaphoreType.DMA((4,)),
            pltpu.SemaphoreType.DMA((4,)),
            pltpu.SemaphoreType.DMA((3,)),
            pltpu.SemaphoreType.DMA((3,)),
        ],
        compiler_params=params(1),
        name="project",
    )(attn, out_proj)


def everyone(n, me):
    mine, across, along, corner = square()
    peers = [{"sp": lax.rem(me + off, n)} for off in range(1, n)]
    return peers + [{"tp": across}, {"tp": along}]


def dispatch_kernel(
    n, chunks, rows_ref, wg_ref, wu_ref, hidden_ref, held, wg, wu, gate, upper, load, send, recv, send_sq, recv_sq
):
    me = lax.axis_index("sp")
    mine, across, along, corner = square()
    parts, _, capacity, depth = held.shape
    width = depth // chunks
    half = width // 2
    rows = n * capacity
    loads = [
        pltpu.make_async_copy(wg_ref.at[0], wg, load.at[0]),
        pltpu.make_async_copy(wu_ref.at[0], wu, load.at[1]),
    ]
    for c in loads:
        c.start()
    own = pltpu.make_async_copy(rows_ref.at[me], held.at[mine, me], load.at[2])
    own.start()
    greet(everyone(n, me), n + 1)

    def span(k, side=0, size=width):
        return pl.ds(pl.multiple_of(k * width + side * half, half), size)

    def scatter(k, off):
        to = lax.rem(me + off, n)
        return remote(
            rows_ref.at[to, :, span(k)],
            held.at[mine, me, :, span(k)],
            send.at[k, off],
            recv.at[k, off],
            {"sp": to},
        )

    def pass_on(k, way):
        group, cols, where = (
            (mine, span(k), across),
            (mine, span(k), along),
            (across, span(k, 0, half), along),
            (along, span(k, 1, half), across),
        )[way]
        ref = held.at[group, :, :, cols]
        return remote(ref, ref, send_sq.at[k, way], recv_sq.at[k, way], {"tp": where})

    @pl.loop(0, chunks)
    def _(k):
        for off in range(1, n):
            scatter(k, off).start()

    for weight in (gate, upper):
        weight[...] = jnp.zeros_like(weight)
    own.wait()
    for c in loads:
        c.wait()

    def absorb_chunk(group, k):
        block = held[group, :, :, span(k)].reshape(rows, width)
        for total, weight in ((gate, wg), (upper, wu)):
            total[group] += jnp.dot(block, weight[span(k), :], preferred_element_type=jnp.float32)

        @pl.when(k == chunks - 1)
        def _():
            act = jax.nn.silu(gate[group]) * upper[group]
            hidden_ref[group] = act.astype(hidden_ref.dtype)

    @pl.loop(0, chunks + 2)
    def _(step):
        @pl.when(step < chunks)
        def _():
            for off in range(1, n):
                scatter(step, off).wait_recv()
            pass_on(step, 0).start()
            pass_on(step, 1).start()

        @pl.when((step >= 1) & (step <= chunks))
        def _():
            for way in (0, 1):
                pass_on(step - 1, way).wait_recv()
                pass_on(step - 1, way + 2).start()

        @pl.when(step < chunks)
        def _():
            absorb_chunk(mine, step)

        @pl.when((step >= 1) & (step <= chunks))
        def _():
            absorb_chunk(across, step - 1)
            absorb_chunk(along, step - 1)

        @pl.when(step >= 2)
        def _():
            for way in (2, 3):
                pass_on(step - 2, way).wait_recv()
            absorb_chunk(corner, step - 2)

    @pl.loop(0, chunks)
    def _(k):
        for off in range(1, n):
            scatter(k, off).wait_send()
        for way in range(4):
            pass_on(k, way).wait_send()


def dispatch(n, parts, rows, w_gate, w_up, chunks=8):
    count, capacity, width = rows.shape
    depth, units = w_gate.shape[1:]
    total = pltpu.VMEM((parts, count * capacity, units), jnp.float32)
    return pl.pallas_call(
        functools.partial(dispatch_kernel, n, chunks),
        out_shape=jax.ShapeDtypeStruct((parts, count * capacity, units), rows.dtype),
        in_specs=in_vmem(1) + [pl.BlockSpec(memory_space=pl.ANY)] * 2,
        out_specs=in_vmem(1)[0],
        scratch_shapes=[
            pltpu.VMEM((parts, count, capacity, width), rows.dtype),
            pltpu.VMEM((depth, units), w_gate.dtype),
            pltpu.VMEM((depth, units), w_up.dtype),
            total,
            total,
            pltpu.SemaphoreType.DMA((3,)),
            pltpu.SemaphoreType.DMA((chunks, n)),
            pltpu.SemaphoreType.DMA((chunks, n)),
            pltpu.SemaphoreType.DMA((chunks, 4)),
            pltpu.SemaphoreType.DMA((chunks, 4)),
        ],
        compiler_params=params(2),
        name="dispatch",
    )(rows, w_gate, w_up)


def combine_kernel(
    n, chunks, hid_ref, wd_ref, out_ref, wd, part, from_x, from_y, to_y, to_x, last_x, last_y, done,
    load, send, recv, send_sq, recv_sq,
):
    me = lax.axis_index("sp")
    mine, across, along, corner = square()
    x, y = lax.rem(mine, 2), mine // 2
    capacity = out_ref.shape[1]
    half = out_ref.shape[2] // chunks // 2
    low, high = pl.ds(0, half), pl.ds(half, half)

    def span(k):
        return pl.ds(pl.multiple_of(2 * k * half, 2 * half), 2 * half)

    def fetch(k):
        return pltpu.make_async_copy(wd_ref.at[0, :, span(k)], wd.at[k], load.at[k])

    @pl.loop(0, chunks)
    def _(k):
        fetch(k).start()

    greet(everyone(n, me), n + 1)

    def hop(k, way):
        src, dst, where = (
            (part.at[k, :, 1 - x, :, low], from_x.at[k], across),
            (part.at[k, 1 - y, :, :, high], from_y.at[k], along),
            (to_y.at[k], last_y.at[k], along),
            (to_x.at[k], last_x.at[k], across),
        )[way]
        return remote(src, dst, send_sq.at[k, way], recv_sq.at[k, way], {"tp": where})

    def home(k, off):
        to = lax.rem(me + off, n)
        return remote(
            done.at[k, to], out_ref.at[me, :, span(k)], send.at[k, off], recv.at[k, off], {"sp": to}
        )

    def wide(value):
        return value.astype(jnp.float32)

    @pl.loop(0, chunks + 2)
    def _(step):
        @pl.when(step < chunks)
        def _(k=step):
            fetch(k).wait()
            for p in range(4):
                product = jnp.dot(hid_ref[p], wd[k], preferred_element_type=jnp.float32)
                part[k, p // 2, p % 2] = product.astype(part.dtype)
            hop(k, 0).start()
            hop(k, 1).start()

        @pl.when((step >= 1) & (step <= chunks))
        def _(k=step - 1):
            hop(k, 0).wait_recv()
            pair = wide(part[k, 1 - y, x, :, low]) + wide(from_x[k, 1 - y])
            to_y[k] = pair.astype(to_y.dtype)
            hop(k, 2).start()
            hop(k, 1).wait_recv()
            pair = wide(part[k, y, 1 - x, :, high]) + wide(from_y[k, 1 - x])
            to_x[k] = pair.astype(to_x.dtype)
            hop(k, 3).start()

        @pl.when(step >= 2)
        def _(k=step - 2):
            hop(k, 2).wait_recv()
            total = wide(part[k, y, x, :, low]) + wide(from_x[k, y]) + wide(last_y[k])
            done[k, :, :, low] = total.astype(done.dtype).reshape(n, capacity, half)
            hop(k, 3).wait_recv()
            total = wide(part[k, y, x, :, high]) + wide(from_y[k, x]) + wide(last_x[k])
            done[k, :, :, high] = total.astype(done.dtype).reshape(n, capacity, half)
            for off in range(1, n):
                home(k, off).start()
            out_ref[me, :, span(k)] = done[k, me]

    @pl.loop(0, chunks)
    def _(k):
        for off in range(1, n):
            home(k, off).wait()
        for way in range(4):
            hop(k, way).wait_send()


def combine(n, hidden, w_down, capacity, chunks=8):
    rows = hidden.shape[1]
    units, width = w_down.shape[1:]
    half = width // chunks // 2
    kind = hidden.dtype
    one = pltpu.VMEM((chunks, rows, half), kind)
    two = pltpu.VMEM((chunks, 2, rows, half), kind)
    return pl.pallas_call(
        functools.partial(combine_kernel, n, chunks),
        out_shape=jax.ShapeDtypeStruct((n, capacity, width), kind),
        in_specs=in_vmem(1) + [pl.BlockSpec(memory_space=pl.ANY)],
        out_specs=in_vmem(1)[0],
        scratch_shapes=[
            pltpu.VMEM((chunks, units, 2 * half), kind),
            pltpu.VMEM((chunks, 2, 2, rows, 2 * half), kind),
            two,
            two,
            one,
            one,
            one,
            one,
            pltpu.VMEM((chunks, n, capacity, 2 * half), kind),
            pltpu.SemaphoreType.DMA((chunks,)),
            pltpu.SemaphoreType.DMA((chunks, n)),
            pltpu.SemaphoreType.DMA((chunks, n)),
            pltpu.SemaphoreType.DMA((chunks, 4)),
            pltpu.SemaphoreType.DMA((chunks, 4)),
        ],
        compiler_params=params(3),
        name="combine",
    )(hidden, w_down)


def start_state(batch, rows, width):
    return (
        jnp.full((batch, rows), NEG_START, jnp.float32),
        jnp.zeros((batch, rows), jnp.float32),
        jnp.zeros((batch, rows, width), jnp.float32),
    )


def local(
    queries,
    keys,
    values,
    query_gain,
    key_gain,
    out_proj,
    expert_norm_scale,
    residual,
    routes,
    route_weights,
    w_gate,
    w_up,
    w_down,
):
    head_size = query_gain.shape[0]
    tok_sp = queries.shape[0]
    tp_count = lax.axis_size("tp")
    sp_count = lax.axis_size("sp")
    heads_dev = queries.shape[1] // head_size
    all_heads = heads_dev * tp_count
    kv_heads = keys.shape[1] // head_size
    group = all_heads // kv_heads
    scale = head_size ** (-0.5)
    tp_index = lax.axis_index("tp")
    sp_index = lax.axis_index("sp")
    position = sp_index * tok_sp + jnp.arange(tok_sp, dtype=jnp.int32)
    q_rot = prepare(queries, query_gain, position)
    shared_value_head = tp_index * heads_dev // group
    own_keys = prepare(
        lax.dynamic_slice_in_dim(keys, shared_value_head * head_size, head_size, 1),
        key_gain,
        position,
    )
    own_values = lax.dynamic_slice_in_dim(values, shared_value_head * head_size, head_size, 1)
    query_matrix = (
        q_rot.reshape(tok_sp, heads_dev, head_size)
        .transpose(1, 0, 2)
        .reshape(1, heads_dev * tok_sp, head_size)
    )
    tok_dev = residual.shape[0]
    top = routes.shape[1]
    capacity = max(2, 2 * tok_dev * top // sp_count)
    direct = tp_count == 4 and sp_count % 2 == 0 and capacity % 16 == 0
    if direct:
        key_piece, value_piece = gather_rows(sp_count, own_keys, own_values)
    else:
        key_piece = lax.all_gather(own_keys, "sp", axis=0, tiled=True)
        value_piece = lax.all_gather(own_values, "sp", axis=0, tiled=True)
    run_max, run_sum, run_acc = absorb(
        start_state(1, heads_dev * tok_sp, head_size),
        query_matrix,
        key_piece[:, None, :],
        value_piece[:, None, :],
        scale,
    )
    attn = (run_acc / run_sum[..., None]).astype(jnp.bfloat16)
    attn = (
        attn.reshape(heads_dev, tok_sp, head_size)
        .transpose(1, 0, 2)
        .reshape(tok_sp, heads_dev * head_size)
    )
    if direct:
        projected = project(attn, out_proj, tok_dev)
    else:
        columns = jnp.dot(
            lax.all_gather(attn, "tp", axis=1, tiled=True),
            out_proj,
            preferred_element_type=jnp.float32,
        )
        projected = lax.all_to_all(
            columns.astype(jnp.bfloat16), "tp", split_axis=0, concat_axis=1, tiled=True
        )
    mixed_float_output = residual.astype(jnp.float32) + projected.astype(jnp.float32)
    mixed = mixed_float_output.astype(jnp.bfloat16)
    mixed_float_output = mixed.astype(jnp.float32)
    normed = (
        mixed_float_output
        * lax.rsqrt(jnp.mean(mixed_float_output * mixed_float_output, axis=-1, keepdims=True) + EPS)
        * expert_norm_scale
    ).astype(jnp.bfloat16)
    flat_routes = routes.reshape(-1)
    one_hot = (flat_routes[:, None] == jnp.arange(sp_count, dtype=jnp.int32)[None, :]).astype(
        jnp.int32
    )
    earlier = jnp.cumsum(one_hot, axis=0) - one_hot
    slot_index = jnp.sum(earlier * one_hot, axis=1)
    target = flat_routes * capacity + slot_index
    selector = (
        jnp.arange(sp_count * capacity, dtype=jnp.int32)[:, None] == target[None, :]
    ).astype(jnp.bfloat16)
    selector = jnp.sum(selector.reshape(sp_count * capacity, tok_dev, top), axis=2)
    send_rows = jnp.dot(selector, normed, preferred_element_type=jnp.float32).astype(jnp.bfloat16)
    if direct:
        hidden = dispatch(
            sp_count,
            tp_count,
            send_rows.reshape(sp_count, capacity, send_rows.shape[1]),
            w_gate,
            w_up,
        )
        returned = combine(sp_count, hidden, w_down, capacity).reshape(send_rows.shape)
        places = jnp.arange(sp_count * capacity, dtype=jnp.int32)[None, None, :]
        chosen = target.reshape(tok_dev, top)[:, :, None] == places
        spread = jnp.sum(jnp.where(chosen, route_weights[:, :, None], 0.0), axis=1)
        coarse = lax.reduce_precision(spread, 8, 7)
        both = jnp.concatenate([coarse, spread - coarse], axis=0).astype(jnp.bfloat16)
        sums = jnp.dot(both, returned, preferred_element_type=jnp.float32)
        return (mixed_float_output + (sums[:tok_dev] + sums[tok_dev:])).astype(jnp.bfloat16)
    arrived = lax.all_to_all(send_rows, "sp", split_axis=0, concat_axis=0, tiled=True)
    piece = lax.all_gather(arrived, "tp", axis=0, tiled=True)
    gate = jnp.dot(piece, w_gate[0], preferred_element_type=jnp.float32)
    upper = jnp.dot(piece, w_up[0], preferred_element_type=jnp.float32)
    hidden = (jax.nn.silu(gate) * upper).astype(jnp.bfloat16)
    partial = jnp.dot(hidden, w_down[0], preferred_element_type=jnp.float32).astype(jnp.bfloat16)
    expert_out = lax.psum_scatter(partial, "tp", scatter_dimension=0, tiled=True)
    returned = lax.all_to_all(expert_out, "sp", split_axis=0, concat_axis=0, tiled=True)
    picked = (
        jnp.take(returned, target, axis=0)
        .astype(jnp.float32)
        .reshape(tok_dev, top, returned.shape[1])
    )
    moe_sum = jnp.sum(picked * route_weights[:, :, None], axis=1)
    return (mixed_float_output + moe_sum).astype(jnp.bfloat16)


def solution(mesh):
    placed = (
        P("sp", "tp"),
        P("sp", None),
        P("sp", None),
        P(),
        P(),
        P(None, "tp"),
        P(),
        P(("sp", "tp"), None),
        P(("sp", "tp"), None),
        P(("sp", "tp"), None),
        P("sp", None, "tp"),
        P("sp", None, "tp"),
        P("sp", "tp", None),
    )
    return jax.shard_map(
        local, mesh=mesh, in_specs=placed, out_specs=P(("sp", "tp"), None), check_vma=False
    )
```
